32 devices in a mesh: grp: 2 (over x), tp: 16 (over z, y, core).
Axes of the slice: x: 2, y: 2, z: 4, core: 2. Of those that a mesh axis runs over, the one named last changes fastest.
Arguments:
- stream_in: bfloat16 [64, 4, 4096], P('grp'), parts along dimension 0, may hold values from -6 to 6
- state_in: float32 [2, 64, 8, 256, 256], P(None, 'grp', None, 'tp'), parts along dimension 1, may hold values from -0.8 to 0.8
- norm_gain: bfloat16 [2, 4096], replicated, may hold values from 0.099609375 to 1.8984375
- query_weight: bfloat16 [2, 4096, 2048], P(None, None, 'tp'), may hold values from -0.09375 to 0.09375
- key_weight: bfloat16 [2, 4096, 2048], P(None, None, 'tp'), may hold values from -0.09375 to 0.09375
- value_weight: bfloat16 [2, 4096, 8, 256], P(None, None, None, 'tp'), as said below
- gate_weight: bfloat16 [2, 4096, 8, 256], P(None, None, None, 'tp'), may hold values from -0.09375 to 0.09375
- group_gain: bfloat16 [2, 8, 256], P(None, None, 'tp'), may hold values from 0.099609375 to 1.8984375
- output_weight: bfloat16 [2, 8, 256, 4096], P(None, None, 'tp'), may hold values from -0.375 to 0.375
Outputs:
- stream_out: bfloat16 [64, 4, 4096], P('grp', None, 'tp'), parts along dimension 0
- state_out: float32 [2, 64, 8, 256, 256], P(None, 'grp', None, 'tp'), parts along dimension 1
The draws below stay inside these ranges and needn't reach their ends.
There are 2 independent parts, one for each index of `grp`. The reference program is written for one: setup_inputs(seed, part) draws one part's arguments, and reference() takes and returns one part's arrays. A program takes and returns all parts, laid end to end along the dimension named above; an argument that names none is the same for every part. Nothing has to cross between parts.
Inputs may be any that keep to these rules, and one draw needn't show every extreme that they name: `value_weight`: real values; column scales of the value projection differ.
All inputs are finite; a program needn't handle non-finite values.
Results may differ from the reference program's by a relative error of at most 0.024.
Values may be sent and summed in bfloat16 or wider, within the bound.
No kernel may reach another device: no remote copies, remote signals or barrier semaphores. Data moves between devices by JAX's collectives and lax.ppermute only.
A program may use at most 64 MiB of HBM per device.

```python
import jax
import jax.numpy as jnp
from jax import lax

D = 4096
HEADS = 8
HEAD_DIM = 256
SEQS = 32
NEW_TOK = 4
PAST = 1024
LAYERS = 2


def draw_value_weight(key, part):
    first_key, second_key = jax.random.split(jax.random.fold_in(key, 17))
    base = jax.random.normal(first_key, (LAYERS, D, HEADS, HEAD_DIM), jnp.float32) * D ** (-0.5)
    ramp = jnp.arange(HEAD_DIM, dtype=jnp.float32) / (HEAD_DIM - 1)
    rough = jax.random.uniform(second_key, (LAYERS, 1, HEADS, HEAD_DIM), jnp.float32, -0.4, 0.4)
    scales = jnp.power(3.0, ramp) * jnp.exp(rough)
    return (base * scales).astype(jnp.bfloat16)


def strengthened(drawn, key, source, target, shards_of, factor):
    def block_of(dim):
        return (jnp.arange(drawn.shape[dim]) // (drawn.shape[dim] // shards_of)).reshape((-1,) + (1,) * (drawn.ndim - 1 - dim))

    near = jax.random.permutation(key, shards_of)[block_of(target)]
    far = (block_of(target) + shards_of // 2) % shards_of
    return jnp.where((block_of(source) == near) | (block_of(source) == far), factor * drawn, drawn)


def level_of(own_key, dims, cuts, smallest, largest):
    loudness, own = 1.0, jax.random.fold_in(own_key, 6)
    for position, blocks in cuts:
        steps = jnp.exp(jax.random.uniform(jax.random.fold_in(own, position), (blocks,), jnp.float32, smallest / len(cuts), largest / len(cuts)))
        loudness = loudness * jnp.repeat(steps, dims[position] // blocks).reshape([-1 if axis == position else 1 for axis in range(len(dims))])
    return loudness


def bell_draw(own_key, shape, scale, most, pieces=(), held_as=jnp.bfloat16):
    factor_of = level_of(own_key, shape, pieces, -0.22, 0.18) if pieces else 1.0
    drawn = jax.random.normal(own_key, shape, jnp.float32) * scale * factor_of
    return jnp.minimum(jnp.maximum(drawn, -most), most).astype(held_as)


def heavy_noise(rng, dims, spread, most, shards, heavy, kind=jnp.bfloat16):
    array = spread * jax.random.normal(rng, dims, jnp.float32)
    if shards:
        array = array * level_of(rng, dims, shards, -0.22, 0.18)
    return jnp.clip(strengthened(array, jax.random.fold_in(rng, 3), *heavy), -most, most).astype(kind)


def setup_inputs(seed: int = 0, part: int = 0) -> dict:
    key_of = jax.random.split(jax.random.key(seed), 10)
    part_splits = jax.random.split(jax.random.fold_in(key_of[9], part), 10)
    return {
        "stream_in": bell_draw(part_splits[0], (SEQS, NEW_TOK, D), 1.0, 6.0),
        "state_in": bell_draw(part_splits[1], (LAYERS, SEQS, HEADS, HEAD_DIM, HEAD_DIM), 0.1, 0.8, ((3, 16),), jnp.float32),
        "norm_gain": jnp.clip(1.0 + 0.18 * jax.random.normal(key_of[2], (LAYERS, D), jnp.float32), 0.099609375, 1.8984375).astype(jnp.bfloat16),
        "query_weight": bell_draw(key_of[3], (LAYERS, D, HEADS * HEAD_DIM), D ** -0.5, 0.09375, ((2, 16),)),
        "key_weight": bell_draw(key_of[4], (LAYERS, D, HEADS * HEAD_DIM), D ** -0.5, 0.09375, ((2, 16),)),
        "value_weight": draw_value_weight(jax.random.fold_in(key_of[9], 71), part),
        "gate_weight": bell_draw(key_of[6], (LAYERS, D, HEADS, HEAD_DIM), D ** -0.5, 0.09375, ((3, 16),)),
        "group_gain": jnp.clip(1.0 + 0.18 * jax.random.normal(key_of[7], (LAYERS, HEADS, HEAD_DIM), jnp.float32), 0.099609375, 1.8984375).astype(jnp.bfloat16),
        "output_weight": heavy_noise(key_of[8], (LAYERS, HEADS, HEAD_DIM, D), (HEADS * HEAD_DIM // 4) ** -0.5, 0.375, ((2, 16),), (2, 3, 16, 2.0)),
    }


EPS_RMS = 1e-06
EPS_GROUP = 1e-05
ROTARY_BASE = 10000.0

def log_decays(count):
    return jnp.log(1.0 - jnp.power(2.0, -5.0 - jnp.arange(count, dtype=jnp.float32)))

def decay_tables(log_gamma, count):
    steps = jnp.arange(count, dtype=jnp.float32)
    gap = steps[:, None] - steps[None, :]
    intra = jnp.where(gap[None] >= 0, jnp.exp(log_gamma[:, None, None] * jnp.maximum(gap, 0.0)[None]), 0.0)
    q_decay = jnp.exp(log_gamma[None, :] * (steps[:, None] + 1.0))
    k_decay = jnp.exp(log_gamma[None, :] * (count - 1.0 - steps[:, None]))
    block_decay = jnp.exp(log_gamma * count)
    return (intra, q_decay, k_decay, block_decay)

def rotate(values, offset):
    half_dim = values.shape[-1] // 2
    freqs = jnp.power(ROTARY_BASE, -jnp.arange(half_dim, dtype=jnp.float32) * (2.0 / values.shape[-1]))
    places = (offset + jnp.arange(values.shape[1])).astype(jnp.float32)
    angles = places[:, None] * freqs[None, :]
    cosine = jnp.cos(angles)[None, :, None, :]
    sine = jnp.sin(angles)[None, :, None, :]
    first = values[..., :half_dim]
    second = values[..., half_dim:]
    return jnp.concatenate([first * cosine - second * sine, second * cosine + first * sine], axis=-1)

def reference(stream_in, state_in, norm_gain, query_weight, key_weight, value_weight, gate_weight, group_gain, output_weight):
    seqs, new_tok, width = stream_in.shape
    heads, head_dim = (value_weight.shape[2], value_weight.shape[3])
    log_gamma = log_decays(heads)
    intra, q_decay, k_decay, block_decay = decay_tables(log_gamma, new_tok)
    highest = lax.Precision.HIGHEST
    stream = stream_in
    new_states = []
    for layer_no in range(state_in.shape[0]):
        stream_f = stream.astype(jnp.float32)
        normed = stream_f * lax.rsqrt(lax.optimization_barrier(jnp.mean(stream_f * stream_f, axis=-1, keepdims=True)) + EPS_RMS)
        normed = (normed * norm_gain[layer_no].astype(jnp.float32)).astype(jnp.bfloat16)
        flat = normed.reshape(seqs * new_tok, width)

        def project(weight):
            result = jnp.dot(flat, weight.reshape(width, heads * head_dim), preferred_element_type=jnp.float32)
            result = lax.optimization_barrier(result.astype(jnp.bfloat16))
            return result.astype(jnp.float32).reshape(seqs, new_tok, heads, head_dim)
        queries = project(query_weight[layer_no])
        key_rows = project(key_weight[layer_no])
        values_f = project(value_weight[layer_no])
        gates_f = project(gate_weight[layer_no])
        rot_q = rotate(queries, PAST)
        rot_k = rotate(key_rows, PAST) * head_dim ** (-0.5)
        scores = jnp.einsum('bthd,bshd->bhts', rot_q, rot_k, precision=highest) * intra[None]
        inner = jnp.einsum('bhts,bshe->bthe', scores, values_f, precision=highest)
        state = state_in[layer_no]
        carried = jnp.einsum('bthd,bhed->bthe', rot_q, state, precision=highest) * q_decay[None, :, :, None]
        mixed = inner + carried
        new_state = state * block_decay[None, :, None, None] + jnp.einsum('bthe,bthd->bhed', values_f, rot_k * k_decay[None, :, :, None], precision=highest)
        mean_o = lax.optimization_barrier(jnp.mean(mixed, axis=-1, keepdims=True))
        var_o = lax.optimization_barrier(jnp.mean(jnp.square(mixed - mean_o), axis=-1, keepdims=True))
        normal = (mixed - mean_o) * lax.rsqrt(var_o + EPS_GROUP) * group_gain[layer_no].astype(jnp.float32)[None, None]
        gated = (jax.nn.silu(gates_f) * normal).astype(jnp.bfloat16)
        branch = jnp.dot(gated.reshape(seqs * new_tok, heads * head_dim), output_weight[layer_no].reshape(heads * head_dim, width), preferred_element_type=jnp.float32)
        stream = (stream.astype(jnp.float32) + branch.reshape(seqs, new_tok, width)).astype(jnp.bfloat16)
        new_states.append(new_state)
    return (stream, jnp.stack(new_states))
```

```python
import functools

import jax
import jax.numpy as jnp
import numpy as np
from jax import lax
from jax.experimental import pallas as pl
from jax.experimental.pallas import tpu as pltpu
from jax.sharding import PartitionSpec as P

HEAD_DIM = 256
PAST = 1024


EPS_RMS = 1e-06
EPS_GROUP = 1e-05
ROTARY_BASE = 10000.0


def log_decays(count):
    return jnp.log(1.0 - jnp.power(2.0, -5.0 - jnp.arange(count, dtype=jnp.float32)))


def decay_tables(log_gamma, count):
    steps = jnp.arange(count, dtype=jnp.float32)
    gap = steps[:, None] - steps[None, :]
    intra = jnp.where(
        gap[None] >= 0, jnp.exp(log_gamma[:, None, None] * jnp.maximum(gap, 0.0)[None]), 0.0
    )
    q_decay = jnp.exp(log_gamma[None, :] * (steps[:, None] + 1.0))
    k_decay = jnp.exp(log_gamma[None, :] * (count - 1.0 - steps[:, None]))
    block_decay = jnp.exp(log_gamma * count)
    return (intra, q_decay, k_decay, block_decay)


def rotate(values, offset):
    half_dim = values.shape[-1] // 2
    freqs = jnp.power(
        ROTARY_BASE, -jnp.arange(half_dim, dtype=jnp.float32) * (2.0 / values.shape[-1])
    )
    places = (offset + jnp.arange(values.shape[1])).astype(jnp.float32)
    angles = places[:, None] * freqs[None, :]
    cosine = jnp.cos(angles)[None, :, None, :]
    sine = jnp.sin(angles)[None, :, None, :]
    first = values[..., :half_dim]
    second = values[..., half_dim:]
    return jnp.concatenate(
        [first * cosine - second * sine, second * cosine + first * sine], axis=-1
    )


def plain_local(
    stream_in,
    state_in,
    norm_gain,
    query_weight,
    key_weight,
    value_weight,
    gate_weight,
    group_gain,
    output_weight,
):
    seqs, new_tok, width = stream_in.shape
    heads, local_dim = (value_weight.shape[2], value_weight.shape[3])
    head_dim = HEAD_DIM
    log_gamma = log_decays(heads)
    intra, q_decay, k_decay, block_decay = decay_tables(log_gamma, new_tok)
    highest = lax.Precision.HIGHEST
    share_cols = width // lax.axis_size("tp")
    col_start = lax.axis_index("tp") * share_cols
    layers = state_in.shape[0]
    stream = stream_in
    stream_share = stream_in
    new_states = []
    for layer_no in range(layers):
        stream_f = stream.astype(jnp.float32)
        normed = stream_f * lax.rsqrt(
            jnp.mean(stream_f * stream_f, axis=-1, keepdims=True) + EPS_RMS
        )
        normed = (normed * norm_gain[layer_no].astype(jnp.float32)).astype(jnp.bfloat16)
        flat = normed.reshape(seqs * new_tok, width)
        query_part = jnp.dot(flat, query_weight[layer_no], preferred_element_type=jnp.float32)
        query_part = query_part.astype(jnp.bfloat16).reshape(seqs, new_tok, -1)
        key_part = jnp.dot(flat, key_weight[layer_no], preferred_element_type=jnp.float32)
        key_part = key_part.astype(jnp.bfloat16).reshape(seqs, new_tok, -1)

        def project_local(weight):
            result = jnp.dot(
                flat, weight.reshape(width, heads * local_dim), preferred_element_type=jnp.float32
            )
            result = lax.optimization_barrier(result.astype(jnp.bfloat16))
            return result.astype(jnp.float32).reshape(seqs, new_tok, heads, local_dim)

        values_f = project_local(value_weight[layer_no])
        gates_f = project_local(gate_weight[layer_no])
        queries, key_rows = (
            lax.all_gather(query_part, "tp", axis=2, tiled=True),
            lax.all_gather(key_part, "tp", axis=2, tiled=True),
        )
        queries = queries.astype(jnp.float32).reshape(seqs, new_tok, heads, head_dim)
        key_rows = key_rows.astype(jnp.float32).reshape(seqs, new_tok, heads, head_dim)
        rot_q = rotate(queries, PAST)
        rot_k = rotate(key_rows, PAST) * head_dim ** (-0.5)
        scores = jnp.einsum("bthd,bshd->bhts", rot_q, rot_k, precision=highest) * intra[None]
        inner = jnp.einsum("bhts,bshe->bthe", scores, values_f, precision=highest)
        state = state_in[layer_no]
        carried = (
            jnp.einsum("bthd,bhed->bthe", rot_q, state, precision=highest)
            * q_decay[None, :, :, None]
        )
        mixed = inner + carried
        new_state = state * block_decay[None, :, None, None] + jnp.einsum(
            "bthe,bthd->bhed", values_f, rot_k * k_decay[None, :, :, None], precision=highest
        )
        new_states.append(new_state)
        totals, squares = lax.psum((jnp.sum(mixed, axis=-1), jnp.sum(mixed * mixed, axis=-1)), "tp")
        mean_o = (totals / head_dim)[..., None]
        var_o = (squares / head_dim)[..., None] - mean_o * mean_o
        normal = (
            (mixed - mean_o)
            * lax.rsqrt(var_o + EPS_GROUP)
            * group_gain[layer_no].astype(jnp.float32)[None, None]
        )
        gated = (jax.nn.silu(gates_f) * normal).astype(jnp.bfloat16)
        partial_out = jnp.dot(
            gated.reshape(seqs * new_tok, heads * local_dim),
            output_weight[layer_no].reshape(heads * local_dim, width),
            preferred_element_type=jnp.float32,
        ).reshape(seqs, new_tok, width)
        share_out = lax.psum_scatter(partial_out, "tp", scatter_dimension=2, tiled=True)
        own_cols = lax.dynamic_slice_in_dim(stream, col_start, share_cols, 2)
        stream_share = (own_cols.astype(jnp.float32) + share_out).astype(jnp.bfloat16)
        if layer_no + 1 < layers:
            stream = lax.all_gather(stream_share, "tp", axis=2, tiled=True)
    result = stream_share
    return (result, jnp.stack(new_states))


BF = jnp.bfloat16
F32 = jnp.float32
VMEM = pltpu.VMEM
NT = (((1,), (1,)), ((), ()))
TN = (((0,), (0,)), ((), ()))


def vspec():
    return pl.BlockSpec(memory_space=VMEM)


def sspec():
    return pl.BlockSpec(memory_space=pltpu.SMEM)


def dot(a, b, dims=(((1,), (0,)), ((), ())), precision=None):
    return lax.dot_general(a, b, dims, precision=precision, preferred_element_type=F32)


def tables(heads, new_tok, head_dim, rows):
    gamma = 1.0 - 2.0 ** (-5.0 - np.arange(heads))
    half = head_dim // 2
    freqs = ROTARY_BASE ** (-np.arange(half) * (2.0 / head_dim))
    tok = np.arange(rows) % new_tok
    angles = (PAST + tok)[:, None] * freqs[None, :]
    up = gamma[:, None, None] ** (tok + 1.0)[None, :, None]
    down = head_dim ** (-0.5) / up
    cos, sin = np.cos(angles)[None], np.sin(angles)[None]
    stacked = np.stack([cos * up, sin * up, cos * down, sin * down], axis=1)
    return stacked.astype(np.float32), (gamma**new_tok).astype(np.float32)


def project_qk_kernel(layer, blocks, jmap, *refs):
    *x_refs, gain_ref, wq_ref, wk_ref, qk_ref, normed_ref = refs
    cols = normed_ref.shape[2]

    def block(p):
        if len(x_refs) == 1:
            return x_refs[0][:, p * cols : (p + 1) * cols].astype(F32)
        each = x_refs[0].shape[0]
        return x_refs[p // each][p % each].astype(F32)

    rows = normed_ref.shape[1]
    lanes = 128
    total = jnp.zeros((rows, lanes), F32)
    for p in range(blocks):
        x = block(p)
        for c in range(0, cols, lanes):
            part = x[:, c : c + lanes]
            total = total + part * part
    scale = lax.rsqrt(jnp.sum(total, axis=1, keepdims=True) / (blocks * cols) + EPS_RMS)
    acc = jnp.zeros(qk_ref.shape, F32)
    for p in range(blocks):
        start = pl.multiple_of(jmap[p] * cols, cols)
        gain = gain_ref[:, pl.ds(start, cols)].astype(F32)[layer : layer + 1]
        normed = (block(p) * scale * gain).astype(BF)
        normed_ref[p] = normed
        weight = jnp.concatenate(
            [wq_ref[layer, pl.ds(start, cols), :], wk_ref[layer, pl.ds(start, cols), :]], axis=1
        )
        acc = acc + dot(normed, weight)
    qk_ref[...] = acc.astype(BF)


def project_vg_kernel(layer, jmap, normed_ref, wv_ref, wg_ref, gain_ref, v_ref, sg_ref):
    blocks, rows, cols = normed_ref.shape
    width = v_ref.shape[1]
    acc = jnp.zeros((rows, 2 * width), F32)
    for p in range(blocks):
        start = pl.multiple_of(jmap[p] * cols, cols)
        weight = jnp.concatenate(
            [wv_ref[layer, :, pl.ds(start, cols)], wg_ref[layer, :, pl.ds(start, cols)]], axis=0
        )
        acc = acc + dot(normed_ref[p], weight, NT)
    v_ref[...] = acc[:, :width].astype(BF)
    gates = acc[:, width:].astype(BF).astype(F32)
    sg_ref[...] = gates / (1.0 + jnp.exp(-gates)) * gain_ref[...].astype(F32)[layer : layer + 1]


def group_masks(shape, heads, per_row, per_lane):
    row = lax.broadcasted_iota(jnp.int32, shape, 0)
    lane = lax.broadcasted_iota(jnp.int32, shape, 1)
    return row // per_row, lane // per_lane


def mix_kernel(dims, pos, own_ref, far_ref, table_ref, v_ref, state_ref, mixed_ref, stats_ref, rk_ref, rq_ref, probs_ref):
    heads, new_tok, head_dim, rows, width, group, trows = dims
    half = head_dim // 2
    local_dim = width // heads
    step = pl.program_id(0)

    @pl.when(step == 0)
    def _():
        row = lax.broadcasted_iota(jnp.int32, (rows, rows), 0)
        col = lax.broadcasted_iota(jnp.int32, (rows, rows), 1)
        allowed = (row // new_tok == col // new_tok) & (row >= col)
        vals = v_ref[...]
        lane_head = lax.broadcasted_iota(jnp.int32, (rows, width), 1) // local_dim
        low = pos[heads] == 0
        parts = []

        def spin(first, second, cos, sin):
            first = first.reshape(rows // trows, trows, half)
            second = second.reshape(rows // trows, trows, half)
            a = first * cos[None] - second * sin[None]
            b = second * cos[None] + first * sin[None]
            return jnp.concatenate([a.reshape(rows, half), b.reshape(rows, half)], axis=1)

        for h in range(heads):
            own = own_ref[pos[h]].astype(F32)
            far = far_ref[pos[h]].astype(F32)
            first = jnp.where(low, own, far)
            second = jnp.where(low, far, own)
            rq = spin(first[:, :half], second[:, :half], table_ref[h, 0], table_ref[h, 1])
            rk = spin(first[:, half:], second[:, half:], table_ref[h, 2], table_ref[h, 3])
            rq_ref[h] = rq
            rk_ref[h] = rk
            scores = dot(rq.astype(BF), rk.astype(BF), NT)
            probs_ref[:, h * rows : (h + 1) * rows] = jnp.where(allowed, scores, 0.0).astype(BF)
            parts.append(jnp.where(lane_head == h, vals.astype(F32), 0.0).astype(BF))
        mixed_ref[...] = dot(probs_ref[...], jnp.concatenate(parts, axis=0))

    pair = 2 * new_tok
    row = lax.broadcasted_iota(jnp.int32, (heads * pair, 2 * width), 0)
    lane = lax.broadcasted_iota(jnp.int32, (heads * pair, 2 * width), 1)
    keep = (row // pair == lane % width // local_dim) & (row % pair // new_tok == lane // width)
    for k in range(group // 2):
        start = pl.multiple_of(step * (group * new_tok) + k * pair, pair)
        left = rq_ref[:, pl.ds(start, pair), :].reshape(heads * pair, head_dim).astype(BF)
        right = state_ref[0, 2 * k : 2 * k + 2].reshape(2 * width, head_dim).astype(BF)
        full = jnp.where(keep, dot(left, right, NT), 0.0)
        summed = jnp.sum(full.reshape(heads, pair, 2 * width), axis=0)
        mixed_ref[pl.ds(start, pair), :] += summed[:, :width] + summed[:, width:]

    @pl.when(step == pl.num_programs(0) - 1)
    def _():
        mixed = mixed_ref[...]
        head, lane = group_masks((heads, width), heads, 1, local_dim)
        pick = (head == lane).astype(F32)
        highest = lax.Precision.HIGHEST
        stats_ref[:heads] = dot(pick, mixed, NT, highest)
        stats_ref[heads:] = dot(pick, mixed * mixed, NT, highest)


def emit_kernel(layer, dims, jmap, mixed_ref, sums_ref, sg_ref, wo_ref, keep_ref, send_ref):
    heads, head_dim, width = dims
    sums = jnp.sum(sums_ref[...], axis=0) * (1.0 / head_dim)
    mean = sums[:heads]
    scale = lax.rsqrt(sums[heads:] - mean * mean + EPS_GROUP)
    head, lane = group_masks((heads, width), heads, 1, width // heads)
    pick = (head == lane).astype(F32)
    highest = lax.Precision.HIGHEST
    normal = (mixed_ref[...] - dot(mean, pick, TN, highest)) * dot(scale, pick, TN, highest)
    gated = (sg_ref[...] * normal).astype(BF)
    each, _, cols = keep_ref.shape
    for p in range(2 * each):
        start = pl.multiple_of(jmap[p] * cols, cols)
        out = dot(gated, wo_ref[layer, :, pl.ds(start, cols)]).astype(BF)
        (keep_ref if p < each else send_ref)[p % each] = out


def update_kernel(dims, fade_ref, v_ref, rk_ref, state_ref, *rest):
    out_ref = rest[-1]
    heads, new_tok, head_dim, width, group = dims
    local_dim = width // heads
    pair = 2 * new_tok
    row = lax.broadcasted_iota(jnp.int32, (heads * pair, 2 * width), 0)
    lane = lax.broadcasted_iota(jnp.int32, (heads * pair, 2 * width), 1)
    keep = (row // pair == lane % width // local_dim) & (row % pair // new_tok == lane // width)
    fade = fade_ref[...]
    vals = v_ref[...].astype(F32)
    for k in range(group // 2):
        v = vals[k * pair : (k + 1) * pair]
        tiled = jnp.broadcast_to(jnp.concatenate([v, v], axis=1)[None], (heads, pair, 2 * width))
        left = jnp.where(keep, tiled.reshape(heads * pair, 2 * width), 0.0).astype(BF)
        right = rk_ref[:, k * pair : (k + 1) * pair, :].reshape(heads * pair, head_dim).astype(BF)
        added = dot(left, right, TN).reshape(2, width, head_dim)
        out_ref[0, 2 * k : 2 * k + 2] = (state_ref[0, 2 * k : 2 * k + 2] + added) * fade[None]


def fast_local(
    stream_in,
    state_in,
    norm_gain,
    query_weight,
    key_weight,
    value_weight,
    gate_weight,
    group_gain,
    output_weight,
):
    seqs, new_tok, width = stream_in.shape
    layers, _, heads, local_dim, head_dim = state_in.shape
    inner = heads * local_dim
    rows = seqs * new_tok
    tp = lax.axis_size("tp")
    cols = width // tp
    deep = tp // 4
    half_blocks = 2 * deep
    me = lax.axis_index("tp").astype(jnp.int32)
    my_core, my_side, my_deep = me % 2, me // 2 % 2, me // 4
    chip = jnp.arange(half_blocks, dtype=jnp.int32)
    place = (my_deep + chip % deep) % deep * 4 + (my_side ^ (chip // deep)) * 2
    jmap = jnp.concatenate([place + my_core, place + (1 - my_core)])
    plain_map = jnp.arange(tp, dtype=jnp.int32)
    head = jnp.arange(heads, dtype=jnp.int32)
    spot = ((head % 2) ^ my_side) * deep + (head // 2 - my_deep) % deep
    pos = jnp.concatenate([spot, my_core[None]])

    group = 8
    trows = 2 * new_tok
    table, fade = tables(heads, new_tok, head_dim, trows)
    fade_rows = jnp.asarray(np.repeat(fade, local_dim)[:, None] * np.ones((1, head_dim), np.float32))
    table = jnp.asarray(table)

    def swap(x, bit):
        return lax.ppermute(x, "tp", [(i, i ^ bit) for i in range(tp)])

    def from_deep(x, p):
        return lax.ppermute(x, "tp", [(i, (i - 4 * p) % tp) for i in range(tp)])

    def to_deep(x, p):
        return lax.ppermute(x, "tp", [(i, (i + 4 * p) % tp) for i in range(tp)])

    def gather(x):
        near = jnp.stack([x] + [from_deep(x, p) for p in range(1, deep)])
        both = jnp.concatenate([near, swap(near, 2)])
        return both, swap(both, 1)

    def total(x):
        x = x + swap(x, 1)
        x = x + swap(x, 2)
        return jnp.stack([x] + [from_deep(x, p) for p in range(1, deep)])

    def add(*parts):
        return sum(part.astype(F32) for part in parts)

    def scatter(keep, send):
        got = swap(send, 1)
        mine = add(keep[:deep], got[:deep]).astype(BF)
        theirs = add(keep[deep:], got[deep:]).astype(BF)
        mine = add(mine, swap(theirs, 2))
        rounded = mine[1:].astype(BF)
        others = [to_deep(rounded[p - 1], p) for p in range(1, deep)]
        return add(mine[0], *others)

    wv = jnp.transpose(value_weight, (0, 2, 3, 1)).reshape(layers, inner, width)
    wg = jnp.transpose(gate_weight, (0, 2, 3, 1)).reshape(layers, inner, width)
    wo = output_weight.reshape(layers, inner, width)
    states = state_in.reshape(layers, seqs, inner, head_dim)
    gains = group_gain.reshape(layers, inner)
    share = lax.dynamic_slice_in_dim(stream_in, me * cols, cols, 2).reshape(rows, cols).astype(F32)
    stream = (stream_in.reshape(rows, width),)
    new_states = None
    for layer in range(layers):
        order = plain_map if layer == 0 else jmap
        qk, normed = pl.pallas_call(
            functools.partial(project_qk_kernel, layer, tp),
            out_shape=(
                jax.ShapeDtypeStruct((rows, 2 * query_weight.shape[2]), BF),
                jax.ShapeDtypeStruct((tp, rows, cols), BF),
            ),
            in_specs=[sspec()] + [vspec()] * (len(stream) + 3),
            out_specs=(vspec(), vspec()),
            name="project_qk",
        )(order, *stream, norm_gain, query_weight, key_weight)
        own, far = gather(qk)
        v, sg = pl.pallas_call(
            functools.partial(project_vg_kernel, layer),
            out_shape=(
                jax.ShapeDtypeStruct((rows, inner), BF),
                jax.ShapeDtypeStruct((rows, inner), F32),
            ),
            in_specs=[sspec()] + [vspec()] * 4,
            out_specs=(vspec(), vspec()),
            cost_estimate=pl.CostEstimate(
                flops=4 * rows * width * inner, bytes_accessed=4 * width * inner, transcendentals=0
            ),
            name="project_vg",
        )(order, normed, wv, wg, gains)
        whole = lambda shape: pl.BlockSpec(shape, lambda i: (0,) * len(shape))
        state_spec = pl.BlockSpec((1, group, inner, head_dim), lambda i: (layer, i, 0, 0))
        mixed, stats, rk = pl.pallas_call(
            functools.partial(
                mix_kernel, (heads, new_tok, head_dim, rows, inner, group, trows)
            ),
            grid=(seqs // group,),
            out_shape=(
                jax.ShapeDtypeStruct((rows, inner), F32),
                jax.ShapeDtypeStruct((2 * heads, rows), F32),
                jax.ShapeDtypeStruct((heads, rows, head_dim), F32),
            ),
            in_specs=[
                sspec(),
                whole(own.shape),
                whole(far.shape),
                whole(table.shape),
                whole(v.shape),
                state_spec,
            ],
            out_specs=(
                whole((rows, inner)),
                whole((2 * heads, rows)),
                whole((heads, rows, head_dim)),
            ),
            scratch_shapes=[
                VMEM((heads, rows, head_dim), F32),
                VMEM((rows, heads * rows), BF),
            ],
            name="mix",
        )(pos, own, far, table, v, states)
        sums = total(stats)
        keep, send = pl.pallas_call(
            functools.partial(emit_kernel, layer, (heads, head_dim, inner)),
            out_shape=(jax.ShapeDtypeStruct((half_blocks, rows, cols), BF),) * 2,
            in_specs=[sspec()] + [vspec()] * 4,
            out_specs=(vspec(), vspec()),
            name="emit",
        )(jmap, mixed, sums, sg, wo)
        share = (share + scatter(keep, send)).astype(BF)
        previous = () if new_states is None else (new_states,)
        new_states = pl.pallas_call(
            functools.partial(update_kernel, (heads, new_tok, head_dim, inner, group)),
            grid=(seqs // group,),
            out_shape=jax.ShapeDtypeStruct(states.shape, F32),
            in_specs=[
                whole(fade_rows.shape),
                pl.BlockSpec((group * new_tok, inner), lambda i: (i, 0)),
                pl.BlockSpec((heads, group * new_tok, head_dim), lambda i: (0, i, 0)),
                state_spec,
            ]
            + [pl.BlockSpec(memory_space=pl.ANY)] * len(previous),
            out_specs=state_spec,
            input_output_aliases={4: 0} if previous else {},
            cost_estimate=pl.CostEstimate(
                flops=2 * seqs * inner * head_dim * 64,
                bytes_accessed=8 * seqs * inner * head_dim,
                transcendentals=0,
            ),
            name="update",
        )(fade_rows, v, rk, states, *previous)
        if layer + 1 < layers:
            stream = gather(share)
            share = share.astype(F32)
    return share.reshape(seqs, new_tok, cols), new_states.reshape(state_in.shape)


def fits(shapes, tp):
    seqs, new_tok, width = shapes[0]
    heads, head_dim = shapes[1][2], shapes[1][4]
    return (
        tp == 2 * heads
        and tp % 4 == 0
        and head_dim == 2 * 128
        and heads * head_dim == 128 * tp
        and new_tok == 4
        and seqs % 8 == 0
        and seqs * new_tok == 128
        and width % (256 * tp) == 0
    )


def local(*args):
    tp = lax.axis_size("tp")
    shapes = [arg.shape for arg in args]
    if fits(shapes, tp):
        return fast_local(*args)
    return plain_local(*args)


def solution(mesh):
    in_specs = (
        P("grp", None, None),
        P(None, "grp", None, "tp", None),
        P(),
        P(None, None, "tp"),
        P(None, None, "tp"),
        P(None, None, None, "tp"),
        P(None, None, None, "tp"),
        P(None, None, "tp"),
        P(None, None, "tp", None),
    )
    out_specs = (P("grp", None, "tp"), P(None, "grp", None, "tp", None))
    return jax.shard_map(local, mesh=mesh, in_specs=in_specs, out_specs=out_specs, check_vma=False)
```
